32 devices in a mesh: ra: 8 (over z, y), cb: 4 (over x, core).
Axes of the slice: x: 2, y: 2, z: 4, core: 2. Of those that a mesh axis runs over, the one named last changes fastest.
Arguments:
- tokens: bfloat16 [1024, 4096], P(None, 'ra'), may hold values from -40 to 40
- norm_gain: float32 [4096], P('ra'), may hold values from 0.1 to 1.9
- gate_weight: bfloat16 [4096, 11264], P('ra', 'cb'), may hold values from -0.09375 to 0.09375
- up_weight: bfloat16 [4096, 11264], P('ra', 'cb'), may hold values from -0.09375 to 0.09375
- down_weight: bfloat16 [11264, 4096], P('cb', 'ra'), may hold values from -0.0546875 to 0.0546875
- out_gain: float32 [4096], P('ra'), may hold values from 0.1 to 1.9
Outputs:
- normed: bfloat16 [1024, 4096], P(None, 'ra')
The draws below stay inside these ranges and needn't reach their ends.
All inputs are finite; a program needn't handle non-finite values.
Results may differ from the reference program's by a relative error of at most 0.0076.
Values may be sent and summed in bfloat16 or wider, within the bound.
No kernel may reach another device: no remote copies, remote signals or barrier semaphores. Data moves between devices by JAX's collectives and lax.ppermute only.
A program may use at most 128 MiB of HBM per device.

```python
import jax
import jax.numpy as jnp
from jax import lax

D = 4096
FF = 11264
TOKENS = 1024


def draw_tokens(key, part):
    keys = jax.random.split(key, 4)
    base = jax.random.normal(keys[0], (TOKENS, D), jnp.float32)
    blocks = jnp.exp(jax.random.uniform(keys[1], (16,), jnp.float32, jnp.log(0.3), jnp.log(3.0)))
    columns = jnp.repeat(blocks, D // 16)[None, :]
    rows = jax.random.uniform(keys[2], (TOKENS, 1), jnp.float32, 0.5, 2.0)
    return jnp.clip(base * columns * rows, -40.0, 40.0).astype(jnp.bfloat16)


def block_scale(key, dims, cuts, smallest, high):
    factor_of = 1.0
    for dim, blocks in cuts:
        heights = jax.random.uniform(jax.random.fold_in(jax.random.fold_in(key, 6), dim), (blocks,), jnp.float32, smallest / len(cuts), high / len(cuts))
        factor_of = factor_of * jnp.repeat(jnp.exp(heights), dims[dim] // blocks).reshape((-1,) + (1,) * (len(dims) - 1 - dim))
    return factor_of


def gaussian(rng, dims, deviation, bound, cuts=(), kind=jnp.bfloat16):
    entries = deviation * jax.random.normal(rng, dims, jnp.float32)
    if cuts:
        entries = entries * block_scale(rng, dims, cuts, -0.22, 0.18)
    return jnp.clip(entries, -bound, bound).astype(kind)


def setup_inputs(seed: int = 0) -> dict:
    key_list = jax.random.split(jax.random.key(seed), 7)
    return {
        "tokens": draw_tokens(jax.random.fold_in(key_list[6], 71), 0),
        "norm_gain": jnp.clip(1.0 + 0.18 * jax.random.normal(key_list[1], (D,), jnp.float32), 0.1, 1.9),
        "gate_weight": gaussian(key_list[2], (D, FF), D ** -0.5, 0.09375, ((0, 8), (1, 4))),
        "up_weight": gaussian(key_list[3], (D, FF), D ** -0.5, 0.09375, ((0, 8), (1, 4))),
        "down_weight": gaussian(key_list[4], (FF, D), FF ** -0.5, 0.0546875, ((0, 4), (1, 8))),
        "out_gain": jnp.clip(1.0 + 0.18 * jax.random.normal(key_list[5], (D,), jnp.float32), 0.1, 1.9),
    }


def reference(tokens, norm_gain, gate_weight, up_weight, down_weight, out_gain):
    stream_in = tokens.astype(jnp.float32)
    inv_rms = jax.lax.rsqrt(lax.optimization_barrier(jnp.sum(stream_in * stream_in, axis=1)) / D + 1e-06)[:, None]
    scaled = (stream_in * norm_gain[None, :]).astype(jnp.bfloat16)
    gate = jnp.dot(scaled, gate_weight, preferred_element_type=jnp.float32) * inv_rms
    up = jnp.dot(scaled, up_weight, preferred_element_type=jnp.float32) * inv_rms
    hidden = (jax.nn.silu(gate) * up).astype(jnp.bfloat16)
    branch = jnp.dot(hidden, down_weight, preferred_element_type=jnp.float32)
    stream = 0.5 * stream_in + branch
    factor = jax.lax.rsqrt(lax.optimization_barrier(jnp.sum(stream * stream, axis=1)) / D + 1e-06)[:, None]
    return (stream * factor * out_gain[None, :]).astype(jnp.bfloat16)
```

```python
import jax
import jax.numpy as jnp
from jax import lax
from jax.sharding import PartitionSpec as P

EPS = 1e-06
F32, BF16 = jnp.float32, jnp.bfloat16
WEIGHTS = (2, 3, 3, 3)
FLIPPED = (2,)


def chunks(width):
    unit = 64 if width % 64 == 0 else width & -width
    tiles, total, edge, cuts = width // unit, sum(WEIGHTS), 0, [0]
    for weight in WEIGHTS:
        edge += weight
        cut = edge * tiles // total
        if cut > cuts[-1]:
            cuts.append(cut)
    return [(a * unit, (b - a) * unit) for a, b in zip(cuts[:-1], cuts[1:])]


def body(cores, tokens, norm_gain, gate_weight, up_weight, down_weight, out_gain):
    rows, features = tokens.shape
    count, nc = lax.axis_size("ra"), cores
    nx = lax.axis_size("cb") // nc
    group = count // 2
    model = features * count
    units, half = gate_weight.shape[1] // group, rows // 2
    ra = lax.axis_index("ra")
    member, low = ra % group, ra < group
    core = lax.axis_index("cb") % nc

    def along_ra(x, mask):
        return lax.ppermute(x, "ra", [(k, k ^ mask) for k in range(count)])

    def along_core(x, shift):
        return lax.ppermute(x, "cb", [(k * nc + j, k * nc + (j + shift) % nc) for k in range(nx) for j in range(nc)])

    def along_x(x, shift):
        return lax.ppermute(x, "cb", [(k * nc + j, (k + shift) % nx * nc + j) for k in range(nx) for j in range(nc)])

    def far_first(x):
        return jnp.where(low, jnp.roll(x, half, axis=0), x)

    share = rows // nc
    scaled = (tokens.astype(F32) * norm_gain[None, :]).astype(BF16)
    part = lax.dynamic_slice_in_dim(tokens, core * share, share, axis=0)
    mine = (part.astype(F32) * norm_gain[None, :]).astype(BF16)
    others = jnp.concatenate([along_ra(mine, s) for s in range(1, group)], axis=1)
    turned = along_core(others, 1)
    far_mine = (core == 1) == low
    others = jnp.where(far_mine, jnp.concatenate([others, turned]), jnp.concatenate([turned, others]))
    inputs = jnp.concatenate([far_first(scaled), others], axis=1)

    stream_in = tokens.astype(F32)
    square = jnp.sum(stream_in * stream_in, axis=1)
    square = square + sum(along_ra(square, s) for s in range(1, group))
    across = along_ra(square, group)
    inv_rms = None

    def columns(weights, owner, start, size):
        at = start * group + owner * size
        return jnp.concatenate([lax.dynamic_slice_in_dim(w, at, size, axis=1) for w in weights], axis=1)

    masks = [1 << k for k in reversed(range(group.bit_length() - 1))]
    weights, last = (gate_weight, up_weight), mine
    branch = jnp.zeros((rows, down_weight.shape[1]), F32)
    for c, (start, size) in enumerate(chunks(units)):
        *weights, last = lax.optimization_barrier((*weights, last))
        messages = [columns(weights, member ^ s, start, size) for s in range(group)]
        last = messages[-1]
        matrix = jnp.concatenate(messages[:1] + [along_ra(messages[s], s) for s in range(1, group)])
        product = jnp.dot(inputs, matrix, preferred_element_type=F32)
        got = along_ra(product[:half].astype(BF16), group)
        if inv_rms is None:
            got, across = lax.optimization_barrier((got, across))
            inv_rms = lax.rsqrt(far_first(square + across)[half:] / model + EPS)[:, None]
        got, scale = lax.optimization_barrier((got, inv_rms))
        total = (product[half:] + got.astype(F32)) * scale
        hidden = (jax.nn.silu(total[:, :size]) * total[:, size:]).astype(BF16)
        other = along_ra(hidden, group)
        hidden = jnp.concatenate([other, hidden])
        owners = [member]
        for mask in masks[::-1] if c in FLIPPED else masks:
            got = along_ra(hidden, mask)
            hidden = jnp.concatenate([hidden, got], axis=1)
            owners = owners + [o ^ mask for o in owners]
        down = jnp.concatenate(
            [lax.dynamic_slice_in_dim(down_weight, start * group + o * size, size, axis=0) for o in owners]
        )
        branch = branch + jnp.dot(hidden, down, preferred_element_type=F32)

    partial = far_first(branch).reshape(nc, share, -1)
    own = lax.dynamic_index_in_dim(partial, core, 0, keepdims=False)
    for turn in range(1, nc):
        other = lax.dynamic_index_in_dim(partial, (core + turn) % nc, 0, keepdims=False)
        own = own + along_core(other.astype(BF16), turn).astype(F32)
    own = own.astype(BF16)
    if nx == 2:
        total = own.astype(F32) + along_x(own, 1).astype(F32)
    else:
        groups = [[k * nc + j for k in range(nx)] for j in range(nc)]
        total = jnp.sum(lax.all_gather(own, "cb", axis_index_groups=groups).astype(F32), axis=0)
    stream = 0.5 * part.astype(F32) + total
    sq = jnp.sum(stream * stream, axis=1)
    mask = 1
    while mask < count:
        sq = sq + along_ra(sq, mask)
        mask *= 2
    factor = lax.rsqrt(sq / model + EPS)[:, None]
    normed = (stream * factor * out_gain[None, :]).astype(BF16)
    turned = along_core(normed, 1)
    return jnp.where(core == 0, jnp.concatenate([normed, turned]), jnp.concatenate([turned, normed]))


def solution(mesh):
    cores = 2
    placed = (P(None, "ra"), P("ra"), P("ra", "cb"), P("ra", "cb"), P("cb", "ra"), P("ra"))

    def step(*arrays):
        return body(cores, *arrays)

    return jax.shard_map(step, mesh=mesh, in_specs=placed, out_specs=P(None, "ra"), check_vma=False)
```
